32 devices in a mesh: sp: 8 (over z, y), tp: 4 (over x, core).
Axes of the slice: x: 2, y: 2, z: 4, core: 2. Of those that a mesh axis runs over, the one named last changes fastest.
Arguments:
- tokens: bfloat16 [4096, 2048], P('sp', 'tp'), may hold values from -400 to 400
- norm_gain: float32 [2048], replicated, may hold values from 0.1 to 1.9
- query_weight: bfloat16 [2048, 1024], P(None, 'tp'), may hold values from -0.37306796 to 0.37306796
- key_weight: bfloat16 [2048, 1024], P(None, 'tp'), may hold values from -0.2625825 to 0.2625825
- value_weight: bfloat16 [2048, 1024], P(None, 'tp'), may hold values from -0.125 to 0.125
- outer_gate_weight: bfloat16 [2048, 1024], P(None, 'tp'), may hold values from -0.125 to 0.125
- inner_gate_weight: bfloat16 [2048, 1024], P(None, 'tp'), may hold values from -0.125 to 0.125
- conv_input_weight: bfloat16 [2048, 1024], P(None, 'tp'), may hold values from -0.125 to 0.125
- conv_taps: float32 [3, 1024], P(None, 'tp'), may hold values from -3.5 to 3.5
- lambdas: float32 [8], P('tp'), may hold values from 0.3 to 0.8
- head_gain: float32 [128], replicated, may hold values from 0.1 to 1.9
- attn_out_weight: bfloat16 [1024, 2048], P(None, 'tp'), may hold values from -0.125 to 0.125
- conv_out_weight: bfloat16 [1024, 2048], P(None, 'tp'), may hold values from -0.125 to 0.125
Outputs:
- mixed_out: bfloat16 [4096, 2048], P('sp', 'tp')
- log_totals: float32 [8, 2, 4096], P('tp', None, 'sp')
The draws below stay inside these ranges and needn't reach their ends.
All inputs are finite; a program needn't handle non-finite values.
Results may differ from the reference program's by a relative error of at most 0.014.
The reference program's roundings to bfloat16 on the way count: a program that leaves them out, or rounds other values in their place, can miss the bound.
Values may be sent and summed in bfloat16 or wider, within the bound.
A program may use at most 128 MiB of HBM per device.

```python
import jax
import jax.numpy as jnp
from jax import lax

WIDTH = 2048
HEADS = 8
HEAD_DIM = 64
TAPS = 3
TOK_DEV = 512
CHANNELS = 1024
TOKENS = 4096


def drawn_weight(key, salt, fan_in):
    base = jax.random.normal(jax.random.fold_in(key, salt), (WIDTH, CHANNELS), jnp.float32)
    base = jnp.clip(base, -6.0, 6.0) * fan_in ** (-0.5)
    return base.astype(jnp.bfloat16)


def draw_query_weight(key, part):
    return drawn_weight(key, 11, WIDTH / 3.0)


def draw_key_weight(key, part):
    return drawn_weight(key, 12, WIDTH * 1.0)


def draw_tokens(key, part):
    values = jnp.clip(jax.random.normal(jax.random.fold_in(key, 2), (TOKENS, WIDTH), jnp.float32), -6.0, 6.0)
    return values.astype(jnp.bfloat16)


def level_of(stream_key, shape, split, low, largest):
    def one(position, parts):
        heights = jax.random.uniform(jax.random.fold_in(jax.random.fold_in(stream_key, 6), position), (parts,), jnp.float32, low / len(split), largest / len(split))
        return jnp.repeat(jnp.exp(heights), shape[position] // parts).reshape((-1,) + (1,) * (len(shape) - position - 1))

    level = one(*split[0])
    for cut in split[1:]:
        level = level * one(*cut)
    return level


def centred(key, dims, spread, most, split=(), held_as=jnp.bfloat16):
    array = jax.random.normal(key, dims, jnp.float32) * spread
    if len(split) > 0:
        array = level_of(key, dims, split, -0.22, 0.18) * array
    return jnp.clip(array, min=-most, max=most).astype(held_as)


def setup_inputs(seed: int = 0) -> dict:
    streams_of = jax.random.split(jax.random.key(seed), 14)
    return {
        "tokens": draw_tokens(jax.random.fold_in(streams_of[13], 71), 0),
        "norm_gain": jnp.clip(1.0 + 0.18 * jax.random.normal(streams_of[1], (WIDTH,), jnp.float32), 0.1, 1.9),
        "query_weight": draw_query_weight(jax.random.fold_in(streams_of[13], 71), 0),
        "key_weight": draw_key_weight(jax.random.fold_in(streams_of[13], 71), 0),
        "value_weight": centred(streams_of[4], (WIDTH, CHANNELS), WIDTH ** -0.5, 0.125, ((1, 4),)),
        "outer_gate_weight": centred(streams_of[5], (WIDTH, CHANNELS), WIDTH ** -0.5, 0.125, ((1, 4),)),
        "inner_gate_weight": centred(streams_of[6], (WIDTH, CHANNELS), WIDTH ** -0.5, 0.125, ((1, 4),)),
        "conv_input_weight": centred(streams_of[7], (WIDTH, CHANNELS), WIDTH ** -0.5, 0.125, ((1, 4),)),
        "conv_taps": centred(streams_of[8], (TAPS, CHANNELS), TAPS ** -0.5, 3.5, ((1, 4),), jnp.float32),
        "lambdas": jnp.clip(0.3 + 0.5 * jax.random.uniform(streams_of[9], (HEADS,), jnp.float32) ** level_of(streams_of[9], (HEADS,), ((0, 4),), -0.2, 0.2), 0.3, 0.8),
        "head_gain": jnp.clip(1.0 + 0.18 * jax.random.normal(streams_of[10], (2 * HEAD_DIM,), jnp.float32), 0.1, 1.9),
        "attn_out_weight": centred(streams_of[11], (CHANNELS, WIDTH), (2 * CHANNELS) ** -0.5, 0.125, ((1, 4),)),
        "conv_out_weight": centred(streams_of[12], (CHANNELS, WIDTH), (2 * CHANNELS) ** -0.5, 0.125, ((1, 4),)),
    }


NORM_EPS = 1e-06
HEAD_EPS = 1e-05
ROPE_BASE = 500000.0
MASKED = -1e+30
HEAD_SCALE = 0.8

def rotate(field_in, positions):
    half_dim = field_in.shape[-1] // 2
    frequency = ROPE_BASE ** (-jnp.arange(half_dim, dtype=jnp.float32) * 2.0 / field_in.shape[-1])
    angles = positions[:, None] * frequency[None, :]
    cosine = jnp.cos(angles)[:, None, None, :]
    sine_part = jnp.sin(angles)[:, None, None, :]
    first_half = field_in[..., :half_dim]
    second_half = field_in[..., half_dim:]
    return jnp.concatenate([first_half * cosine - second_half * sine_part, second_half * cosine + first_half * sine_part], axis=-1)

def reference(tokens, norm_gain, query_weight, key_weight, value_weight, outer_gate_weight, inner_gate_weight, conv_input_weight, conv_taps, lambdas, head_gain, attn_out_weight, conv_out_weight):
    floats = tokens.astype(jnp.float32)
    inverse_rms = lax.rsqrt(lax.optimization_barrier(jnp.mean(floats * floats, axis=1, keepdims=True)) + NORM_EPS)
    scaled = (floats * norm_gain[None, :]).astype(jnp.bfloat16)

    def project(weight):
        return inverse_rms * jnp.dot(scaled, weight, preferred_element_type=jnp.float32)
    positions = jnp.arange(TOKENS, dtype=jnp.float32)
    queries = rotate(project(query_weight).reshape(TOKENS, HEADS, 2, HEAD_DIM), positions).astype(jnp.bfloat16)
    key_rows = rotate(project(key_weight).reshape(TOKENS, HEADS, 2, HEAD_DIM), positions).astype(jnp.bfloat16)
    values = project(value_weight).astype(jnp.bfloat16).reshape(TOKENS, HEADS, 2 * HEAD_DIM)
    outer_gate = project(outer_gate_weight).astype(jnp.bfloat16)
    inner_gate = project(inner_gate_weight).astype(jnp.bfloat16)
    signal = project(conv_input_weight).astype(jnp.bfloat16)
    conv_in = (inner_gate.astype(jnp.float32) * signal.astype(jnp.float32)).astype(jnp.bfloat16)
    padded = jnp.concatenate([jnp.zeros((TAPS - 1, CHANNELS), jnp.bfloat16), conv_in], axis=0)
    summed = jnp.zeros((TOKENS, CHANNELS), jnp.float32)
    for tap_index in range(TAPS):
        summed = summed + conv_taps[tap_index][None, :] * padded[tap_index:tap_index + TOKENS].astype(jnp.float32)
    conv_out = (outer_gate.astype(jnp.float32) * summed).astype(jnp.bfloat16)
    blocks = TOKENS // TOK_DEV

    def one_block(flat_index):
        head_index = flat_index // blocks
        row_start = (flat_index % blocks * TOK_DEV).astype(jnp.int32)
        query_rows = lax.dynamic_slice_in_dim(queries, row_start, TOK_DEV, 0)
        query_rows = lax.dynamic_index_in_dim(query_rows, head_index, 1, keepdims=False)
        head_keys = lax.dynamic_index_in_dim(key_rows, head_index, 1, keepdims=False)
        head_values = lax.dynamic_index_in_dim(values, head_index, 1, keepdims=False)
        scores = jnp.einsum('qcd,kcd->cqk', query_rows.astype(jnp.float32), head_keys.astype(jnp.float32)) * HEAD_DIM ** (-0.5)
        visible = (row_start + jnp.arange(TOK_DEV, dtype=jnp.int32))[:, None] >= jnp.arange(TOKENS, dtype=jnp.int32)[None, :]
        scores = jnp.where(visible[None], scores, MASKED)
        row_max = lax.optimization_barrier(jnp.max(scores, axis=-1, keepdims=True))
        exponent = jnp.where(visible[None], jnp.exp(scores - row_max), 0.0)
        row_sum = lax.optimization_barrier(jnp.sum(exponent, axis=-1, keepdims=True))
        normalized = exponent / row_sum
        lambda_value = lambdas[head_index]
        weights = (normalized[0] - lambda_value * normalized[1]).astype(jnp.bfloat16)
        head_mix = jnp.dot(weights, head_values, preferred_element_type=jnp.float32)
        normed = head_mix * lax.rsqrt(lax.optimization_barrier(jnp.mean(head_mix * head_mix, axis=-1, keepdims=True)) + HEAD_EPS) * head_gain[None, :] * HEAD_SCALE
        return (normed.astype(jnp.bfloat16), (row_max + jnp.log(row_sum))[..., 0])
    head_rows, log_rows = lax.map(one_block, jnp.arange(HEADS * blocks, dtype=jnp.int32))
    attn_out = jnp.transpose(head_rows.reshape(HEADS, blocks, TOK_DEV, 2 * HEAD_DIM), (1, 2, 0, 3)).reshape(TOKENS, CHANNELS)
    log_totals = jnp.transpose(log_rows.reshape(HEADS, blocks, 2, TOK_DEV), (0, 2, 1, 3)).reshape(HEADS, 2, TOKENS)
    mixed_out = jnp.dot(attn_out, attn_out_weight, preferred_element_type=jnp.float32) + jnp.dot(conv_out, conv_out_weight, preferred_element_type=jnp.float32)
    return (mixed_out.astype(jnp.bfloat16), log_totals)
```

```python
import functools

import jax
import jax.numpy as jnp
from jax import lax
from jax.experimental import pallas as pl
from jax.experimental.pallas import tpu as pltpu
from jax.sharding import PartitionSpec as P

NORM_EPS = 1e-06
HEAD_EPS = 1e-05
ROPE_BASE = 500000.0
MASKED = -1e30
HEAD_SCALE = 0.8
F32 = jnp.float32
BF16 = jnp.bfloat16


def dot(a, b):
    return jnp.dot(a, b, preferred_element_type=F32)


def dot_t(a, b):
    return lax.dot_general(a, b, (((1,), (1,)), ((), ())), preferred_element_type=F32)


def kernel(
    dims,
    tokens,
    gain,
    freq,
    wq_h,
    wk_h,
    wv_h,
    wo_h,
    wi_h,
    ws_h,
    taps,
    lambdas,
    head_gain,
    wa_h,
    wc_h,
    out,
    lse,
    tok,
    scaled,
    inv,
    cos_t,
    sin_t,
    wq,
    wk,
    wv,
    wo,
    wi,
    ws,
    wa,
    wc,
    kv,
    qz,
    row_max,
    row_sum,
    acc,
    gate,
    padded,
    tail,
    rim,
    conv_all,
    attn_all,
    total,
    w_sem,
    own_sem,
    tok_recv,
    tok_send,
    tok_relay,
    kv_recv,
    kv_send_z,
    kv_send_y,
    rim_sem,
    mix_recv,
    mix_send,
    mix_relay,
):
    S, T, Z, Y, H = dims["S"], dims["T"], dims["Z"], dims["Y"], dims["H"]
    L, Dt = tokens.shape
    Wd = T * Dt
    C = wq_h.shape[1]
    V = C // H
    hd = V // 2
    NR = tok_recv.shape[1]
    R = L // NR
    NM = mix_recv.shape[2]
    M = L // NM
    X = T // 2
    taps_n = taps.shape[0]
    PAD = tail.shape[0]

    sp = lax.axis_index("sp")
    tp = lax.axis_index("tp")
    z = sp // Y
    y = sp % Y
    core = tp % 2
    xi = tp // 2
    sib = xi * 2 + (1 - core)

    def peer(k):
        return ((xi + k) % X) * 2 + core

    def source(k):
        return ((xi - k + X) % X) * 2 + core

    pairs = [(wk_h, wk), (wv_h, wv), (wq_h, wq), (wi_h, wi), (ws_h, ws), (wo_h, wo), (wc_h, wc), (wa_h, wa)]
    own = pltpu.make_async_copy(tokens, tok.at[tp], own_sem)
    own.start()
    loads = [pltpu.make_async_copy(s, d, w_sem.at[i]) for i, (s, d) in enumerate(pairs)]
    for load in loads:
        load.start()

    barrier = pltpu.get_barrier_semaphore()

    def greet(target):
        pl.semaphore_signal(barrier, inc=1, device_id=target)

    for k in range(1, T):
        greet({"tp": (tp + k) % T})
    for k in range(1, Y):
        greet({"sp": z * Y + (y + k) % Y})
    has_up = z + 1 < Z
    has_down = z > 0
    far_up = jnp.logical_and(has_up, y == Y - 1) if Y > 1 else None
    far_down = jnp.logical_and(has_down, y == 0) if Y > 1 else None
    expect = (T - 1) + (Y - 1) + has_up.astype(jnp.int32) + has_down.astype(jnp.int32)

    @pl.when(has_up)
    def _():
        greet({"sp": sp + Y})

    @pl.when(has_down)
    def _():
        greet({"sp": sp - Y})

    if Y > 1:
        expect = expect + far_up.astype(jnp.int32) + far_down.astype(jnp.int32)

        @pl.when(far_up)
        def _():
            greet({"sp": sp + 1})

        @pl.when(far_down)
        def _():
            greet({"sp": sp - 1})

    pl.semaphore_wait(barrier, expect)

    def tok_rows(r):
        return pl.ds(pl.multiple_of(r * R, R), R)

    def tok_copy(src, piece, r, send, target):
        return pltpu.make_async_remote_copy(
            src_ref=src,
            dst_ref=tok.at[piece, tok_rows(r), :],
            send_sem=send,
            recv_sem=tok_recv.at[piece, r],
            device_id={"tp": target},
        )

    def tok_own(k, r):
        target = peer(k) if k else sib
        return tok_copy(tokens.at[tok_rows(r), :], tp, r, tok_send.at[k, r], target)

    def tok_forward(k, r):
        piece = source(k)
        return tok_copy(tok.at[piece, tok_rows(r), :], piece, r, tok_relay.at[k, r], sib)

    def tok_wait(piece, r):
        tok_copy(tok.at[piece, tok_rows(r), :], piece, r, tok_send.at[0, r], sib).wait_recv()

    for r in range(NR):
        for k in list(range(1, X)) + [0]:
            tok_own(k, r).start()

    lane = lax.broadcasted_iota(jnp.int32, (R, V), 1)
    first = (lane % hd) < (hd // 2)

    def table(r, carry):
        base = sp * L + r * R
        pos = (base + lax.broadcasted_iota(jnp.int32, (R, V), 0)).astype(F32)
        angle = pos * freq[...]
        sine = jnp.sin(angle)
        cos_t[tok_rows(r), :] = jnp.cos(angle)
        sin_t[tok_rows(r), :] = jnp.where(first, -sine, sine)
        return carry

    lax.fori_loop(0, NR, table, 0)

    def rotate(block, rows):
        low = (lax.broadcasted_iota(jnp.int32, block.shape, 1) % hd) < (hd // 2)
        other = jnp.where(
            low, pltpu.roll(block, V - hd // 2, 1), pltpu.roll(block, hd // 2, 1)
        )
        return block * cos_t[rows, :] + other * sin_t[rows, :]

    def kv_copy(j, r, send, target):
        block = kv.at[j, tok_rows(r), :]
        return pltpu.make_async_remote_copy(
            src_ref=block,
            dst_ref=block,
            send_sem=send,
            recv_sem=kv_recv.at[j, r],
            device_id={"sp": target},
        )

    def kv_up(dz, r):
        return kv_copy(sp - dz * Y, r, kv_send_z.at[dz, r], sp + Y)

    def kv_side(dz, r, k):
        return kv_copy(sp - dz * Y, r, kv_send_y.at[dz, r, k - 1], z * Y + (y + k) % Y)

    def kv_wait(j, r):
        kv_copy(j, r, kv_send_z.at[0, r], sp).wait_recv()

    def kv_send(dz, r, act):
        @pl.when(has_up)
        def _():
            act(kv_up(dz, r))

        for k in range(1, Y):

            @pl.when(jnp.logical_or(dz > 0, y + k < Y))
            def _():
                act(kv_side(dz, r, k))

    own.wait()
    loads[0].wait()
    loads[1].wait()

    def key_chunk(r, carry):
        rows = tok_rows(r)
        for k in range(1, X):
            tok_wait(source(k), r)
            tok_forward(k, r).start()
        tok_wait(sib, r)
        for k in range(1, X):
            tok_wait(((xi + k) % X) * 2 + (1 - core), r)
        squares = jnp.zeros((R, 1), F32)
        for t in range(T):
            block = tok[t, rows, :].astype(F32)
            squares = squares + jnp.sum(block * block, axis=1, keepdims=True)
            scaled[rows, t * Dt : (t + 1) * Dt] = (block * gain[t : t + 1, :]).astype(BF16)
        inverse = lax.rsqrt(squares / Wd + NORM_EPS)
        inv[rows, :] = inverse
        left = scaled[rows, :]
        keys = inverse * dot(left, wk[...])
        for h in range(H):
            kv[sp, rows, h * V : (h + 1) * V] = rotate(keys[:, h * V : (h + 1) * V], rows).astype(BF16)
        kv[sp, rows, C : 2 * C] = (inverse * dot(left, wv[...])).astype(BF16)
        kv_send(0, r, lambda copy: copy.start())
        return carry

    lax.fori_loop(0, NR, key_chunk, 0)

    for load in loads[2:6]:
        load.wait()
    half = lax.broadcasted_iota(jnp.int32, (M, V), 1) < hd
    scale = hd ** (-0.5)

    def mix_rows(r):
        return pl.ds(pl.multiple_of(r * M, M), M)

    def query_chunk(r, carry):
        rows = mix_rows(r)
        inverse = inv[rows, :]
        left = scaled[rows, :]
        queries = inverse * dot(left, wq[...])
        for h in range(H):
            turned = rotate(queries[:, h * V : (h + 1) * V], rows).astype(BF16).astype(F32) * scale
            qz[h, 0, rows, :] = jnp.where(half, turned, 0.0).astype(BF16)
            qz[h, 1, rows, :] = jnp.where(half, 0.0, turned).astype(BF16)
        inner = (inverse * dot(left, wi[...])).astype(BF16)
        signal = (inverse * dot(left, ws[...])).astype(BF16)
        conv_in = (inner.astype(F32) * signal.astype(F32)).astype(BF16)
        padded[pl.ds(pl.multiple_of(PAD + r * M, PAD), M), :] = conv_in.astype(F32)
        gate[rows, :] = (inverse * dot(left, wo[...])).astype(BF16)
        return carry

    lax.fori_loop(0, NM, query_chunk, 0)
    tail[...] = padded[L : L + PAD, :].astype(BF16)
    rim_copy = pltpu.make_async_remote_copy(
        src_ref=tail,
        dst_ref=rim,
        send_sem=rim_sem.at[0],
        recv_sem=rim_sem.at[1],
        device_id={"sp": (sp + 1) % S},
    )

    @pl.when(sp + 1 < S)
    def _():
        rim_copy.start()

    def attend(j, diagonal):
        def one(i, carry):
            rows = mix_rows(i)
            for h in range(H):
                query = qz[h, :, rows, :].reshape(2 * M, V)
                scores = dot_t(query, kv[j, :, h * V : (h + 1) * V])
                if diagonal:
                    row = lax.broadcasted_iota(jnp.int32, scores.shape, 0)
                    row = jnp.where(row >= M, row - M, row) + i * M
                    col = lax.broadcasted_iota(jnp.int32, scores.shape, 1)
                    scores = jnp.where(row >= col, scores, MASKED)
                    new_max = jnp.max(scores, axis=1, keepdims=True)
                else:
                    old_max = row_max[h, :, rows, :].reshape(2 * M, 1)
                    new_max = jnp.maximum(old_max, jnp.max(scores, axis=1, keepdims=True))
                weights = jnp.exp(scores - new_max)
                sums = jnp.sum(weights, axis=1, keepdims=True)
                mixed = dot(weights.astype(BF16), kv[j, :, C + h * V : C + (h + 1) * V])
                if not diagonal:
                    fade = jnp.exp(old_max - new_max)
                    sums = sums + fade * row_sum[h, :, rows, :].reshape(2 * M, 1)
                    mixed = mixed + fade * acc[h, :, rows, :].reshape(2 * M, V)
                row_max[h, :, rows, :] = new_max.reshape(2, M, 1)
                row_sum[h, :, rows, :] = sums.reshape(2, M, 1)
                acc[h, :, rows, :] = mixed.reshape(2, M, V)
            return carry

        lax.fori_loop(0, NM, one, 0)

    attend(sp, True)

    @pl.when(sp > 0)
    def _():
        rim_copy.wait_recv()
        padded[0:PAD, :] = rim[...].astype(F32)

    @pl.when(sp == 0)
    def _():
        padded[0:PAD, :] = jnp.zeros((PAD, C), F32)

    summed = jnp.zeros((L, C), F32)
    for j in range(taps_n):
        begin = PAD - (taps_n - 1) + j
        summed = summed + taps[j : j + 1, :] * padded[begin : begin + L, :]
    conv_all[tp, :, :] = (gate[...].astype(F32) * summed).astype(BF16)

    def mix_copy(which, buf, piece, r, send, target):
        block = buf.at[piece, mix_rows(r), :]
        return pltpu.make_async_remote_copy(
            src_ref=block,
            dst_ref=block,
            send_sem=send,
            recv_sem=mix_recv.at[which, piece, r],
            device_id={"tp": target},
        )

    def mix_own(which, buf, k, r):
        target = peer(k) if k else sib
        return mix_copy(which, buf, tp, r, mix_send.at[which, k, r], target)

    def mix_forward(which, buf, k, r):
        return mix_copy(which, buf, source(k), r, mix_relay.at[which, k, r], sib)

    def mix_wait(which, buf, piece, r):
        mix_copy(which, buf, piece, r, mix_send.at[which, 0, r], sib).wait_recv()

    for r in range(NM):
        for k in list(range(1, X)) + [0]:
            mix_own(0, conv_all, k, r).start()

    def step(dz, carry):
        @pl.when(dz <= z)
        def _():
            def forward(r, inner):
                kv_wait(sp - dz * Y, r)
                kv_send(dz, r, lambda copy: copy.start())
                return inner

            lax.fori_loop(0, NR, forward, 0)

        def row_block(k, inner):
            side = (y + k) % Y
            level = jnp.where(k == 0, z - dz, z - dz + 1)
            j = level * Y + side
            valid = jnp.where(k == 0, dz <= z, jnp.logical_or(level < z, side < y))

            @pl.when(valid)
            def _():
                @pl.when(k > 0)
                def _():
                    for r in range(NR):
                        kv_wait(j, r)

                attend(j, False)

            return inner

        lax.fori_loop(0, Y, row_block, 0)
        return carry

    lax.fori_loop(1, z + 2, step, 0)

    def finish(i, carry):
        rows = mix_rows(i)
        for h in range(H):
            first_map = acc[h, 0, rows, :] / row_sum[h, 0, rows, :]
            second_map = acc[h, 1, rows, :] / row_sum[h, 1, rows, :]
            head_mix = first_map - lambdas[h] * second_map
            mean = jnp.mean(head_mix * head_mix, axis=1, keepdims=True)
            normed = head_mix * lax.rsqrt(mean + HEAD_EPS) * head_gain[...] * HEAD_SCALE
            attn_all[tp, rows, h * V : (h + 1) * V] = normed.astype(BF16)
        for k in list(range(1, X)) + [0]:
            mix_own(1, attn_all, k, i).start()
        return carry

    lax.fori_loop(0, NM, finish, 0)

    loads[6].wait()
    loads[7].wait()

    def gather(which, buf, r):
        for k in range(1, X):
            mix_wait(which, buf, source(k), r)
            mix_forward(which, buf, k, r).start()

    def gather_rest(which, buf, r):
        mix_wait(which, buf, sib, r)
        for k in range(1, X):
            mix_wait(which, buf, ((xi + k) % X) * 2 + (1 - core), r)

    def conv_part(r, carry):
        rows = mix_rows(r)
        gather(0, conv_all, r)
        gather_rest(0, conv_all, r)
        part = dot(conv_all[0, rows, :], wc[0:C, :])
        for t in range(1, T):
            part = part + dot(conv_all[t, rows, :], wc[t * C : (t + 1) * C, :])
        total[rows, :] = part
        return carry

    lax.fori_loop(0, NM, conv_part, 0)

    lanes = lax.broadcasted_iota(jnp.int32, (L, 128), 1)
    columns = jnp.zeros((L, 128), F32)
    for h in range(H):
        for c in range(2):
            value = row_max[h, c, :, :] + jnp.log(row_sum[h, c, :, :])
            columns = jnp.where(lanes == 2 * h + c, value, columns)
    lse[...] = jnp.transpose(columns)[0 : 2 * H, :]

    def attn_part(r, carry):
        rows = mix_rows(r)
        gather(1, attn_all, r)
        gather_rest(1, attn_all, r)
        part = total[rows, :]
        for t in range(T):
            part = part + dot(attn_all[t, rows, :], wa[t * C : (t + 1) * C, :])
        out[rows, :] = part.astype(BF16)
        return carry

    lax.fori_loop(0, NM, attn_part, 0)

    for r in range(NR):
        for k in range(X):
            tok_own(k, r).wait_send()
        for k in range(1, X):
            tok_forward(k, r).wait_send()

    def drain(dz, carry):
        def inner(r, c):
            kv_send(dz, r, lambda copy: copy.wait_send())
            return c

        return lax.fori_loop(0, NR, inner, carry)

    lax.fori_loop(0, z + 1, drain, 0)
    for which, buf in ((0, conv_all), (1, attn_all)):
        for r in range(NM):
            for k in range(X):
                mix_own(which, buf, k, r).wait_send()
            for k in range(1, X):
                mix_forward(which, buf, k, r).wait_send()

    @pl.when(sp + 1 < S)
    def _():
        rim_copy.wait_send()


def per_device(
    dims,
    tokens,
    norm_gain,
    query_weight,
    key_weight,
    value_weight,
    outer_gate_weight,
    inner_gate_weight,
    conv_input_weight,
    conv_taps,
    lambdas,
    head_gain,
    attn_out_weight,
    conv_out_weight,
):
    S, T, Z, Y = dims["S"], dims["T"], dims["Z"], dims["Y"]
    L, Dt = tokens.shape
    H = lambdas.shape[0]
    C = query_weight.shape[1]
    V = C // H
    hd = V // 2
    O = attn_out_weight.shape[1]
    Wd = norm_gain.shape[0]
    NR, NM, PAD = 4, 2, 16
    X = T // 2
    frequency = ROPE_BASE ** (-jnp.arange(hd // 2, dtype=F32) * 2.0 / hd)
    freq = jnp.tile(frequency, 4)[None, :]
    any_spec = pl.BlockSpec(memory_space=pl.ANY)
    vmem = pl.BlockSpec(memory_space=pltpu.VMEM)
    smem = pl.BlockSpec(memory_space=pltpu.SMEM)
    dma = pltpu.SemaphoreType.DMA
    mixed, lse = pl.pallas_call(
        functools.partial(kernel, dict(dims, H=H)),
        out_shape=(
            jax.ShapeDtypeStruct((L, O), BF16),
            jax.ShapeDtypeStruct((2 * H, L), F32),
        ),
        in_specs=[any_spec, vmem, vmem] + [any_spec] * 6 + [vmem, smem, vmem] + [any_spec] * 2,
        out_specs=(vmem, vmem),
        scratch_shapes=[
            pltpu.VMEM((T, L, Dt), BF16),
            pltpu.VMEM((L, Wd), BF16),
            pltpu.VMEM((L, 1), F32),
            pltpu.VMEM((L, V), F32),
            pltpu.VMEM((L, V), F32),
        ]
        + [pltpu.VMEM((Wd, C), BF16)] * 6
        + [pltpu.VMEM((T * C, O), BF16)] * 2
        + [
            pltpu.VMEM((S, L, 2 * C), BF16),
            pltpu.VMEM((H, 2, L, V), BF16),
            pltpu.VMEM((H, 2, L, 1), F32),
            pltpu.VMEM((H, 2, L, 1), F32),
            pltpu.VMEM((H, 2, L, V), F32),
            pltpu.VMEM((L, C), BF16),
            pltpu.VMEM((PAD + L, C), F32),
            pltpu.VMEM((PAD, C), BF16),
            pltpu.VMEM((PAD, C), BF16),
            pltpu.VMEM((T, L, C), BF16),
            pltpu.VMEM((T, L, C), BF16),
            pltpu.VMEM((L, O), F32),
            dma((8,)),
            dma,
            dma((T, NR)),
            dma((X, NR)),
            dma((X, NR)),
            dma((S, NR)),
            dma((Z, NR)),
            dma((Z, NR, max(Y - 1, 1))),
            dma((2,)),
            dma((2, T, NM)),
            dma((2, X, NM)),
            dma((2, X, NM)),
        ],
        compiler_params=pltpu.CompilerParams(
            collective_id=0, has_side_effects=True, vmem_limit_bytes=60 * 1024 * 1024
        ),
        name="mixer",
    )(
        tokens,
        norm_gain.reshape(T, Dt),
        freq,
        query_weight,
        key_weight,
        value_weight,
        outer_gate_weight,
        inner_gate_weight,
        conv_input_weight,
        conv_taps,
        lambdas,
        head_gain[None, :],
        attn_out_weight,
        conv_out_weight,
    )
    return mixed, lse.reshape(H, 2, L)


def solution(mesh):
    S, T = mesh.shape["sp"], mesh.shape["tp"]
    Y = max(d for d in range(1, S + 1) if S % d == 0 and d * d <= S)
    dims = {"S": S, "T": T, "Z": S // Y, "Y": Y}
    in_specs = (
        P("sp", "tp"),
        P(),
        P(None, "tp"),
        P(None, "tp"),
        P(None, "tp"),
        P(None, "tp"),
        P(None, "tp"),
        P(None, "tp"),
        P(None, "tp"),
        P("tp"),
        P(),
        P(None, "tp"),
        P(None, "tp"),
    )
    out_specs = (P("sp", "tp"), P("tp", None, "sp"))
    return jax.shard_map(
        functools.partial(per_device, dims),
        mesh=mesh,
        in_specs=in_specs,
        out_specs=out_specs,
        check_vma=False,
    )
```

```python
import functools

import jax
import jax.numpy as jnp
import numpy as np
from jax import lax
from jax.experimental import pallas as pl
from jax.experimental.pallas import tpu as pltpu
from jax.sharding import PartitionSpec as P

NORM_EPS = 1e-06
HEAD_EPS = 1e-05
ROPE_BASE = 500000.0
MASKED = -1e30
HEAD_SCALE = 0.8
F32 = jnp.float32
BF16 = jnp.bfloat16


def dot(a, b):
    return jnp.dot(a, b, preferred_element_type=F32)


def dot_t(a, b):
    return lax.dot_general(a, b, (((1,), (1,)), ((), ())), preferred_element_type=F32)


def kernel(
    dims,
    tokens,
    gain,
    freq,
    wq_h,
    wk_h,
    wv_h,
    wo_h,
    wi_h,
    ws_h,
    taps,
    lambdas,
    head_gain,
    wa_h,
    wc_h,
    out,
    lse,
    tok,
    scaled,
    inv,
    cos_t,
    sin_t,
    wq,
    wk,
    wv,
    wo,
    wi,
    ws,
    wa,
    wc,
    kv,
    qz,
    row_max,
    row_sum,
    acc,
    gate,
    padded,
    tail,
    rim,
    conv_all,
    attn_all,
    total,
    w_sem,
    own_sem,
    tok_recv,
    tok_send,
    tok_relay,
    kv_recv,
    kv_send_z,
    kv_send_y,
    kv_extra,
    rim_sem,
    mix_recv,
    mix_send,
    mix_relay,
):
    S, T, Z, Y, H = dims["S"], dims["T"], dims["Z"], dims["Y"], dims["H"]
    L, Dt = tokens.shape
    Wd = T * Dt
    C = wq_h.shape[1]
    V = C // H
    hd = V // 2
    NR = tok_recv.shape[1]
    R = L // NR
    NM = mix_recv.shape[2]
    M = L // NM
    X = T // 2
    taps_n = taps.shape[0]
    PAD = tail.shape[0]

    sp = lax.axis_index("sp")
    tp = lax.axis_index("tp")
    z = sp // Y
    y = sp % Y
    core = tp % 2
    xi = tp // 2
    sib = xi * 2 + (1 - core)

    def peer(k):
        return ((xi + k) % X) * 2 + core

    def source(k):
        return ((xi - k + X) % X) * 2 + core

    pairs = [(wk_h, wk), (wv_h, wv), (wq_h, wq), (wi_h, wi), (ws_h, ws), (wo_h, wo), (wc_h, wc), (wa_h, wa)]
    own = pltpu.make_async_copy(tokens, tok.at[tp], own_sem)
    own.start()
    loads = [pltpu.make_async_copy(s, d, w_sem.at[i]) for i, (s, d) in enumerate(pairs)]
    for load in loads:
        load.start()

    barrier = pltpu.get_barrier_semaphore()

    def greet(target):
        pl.semaphore_signal(barrier, inc=1, device_id=target)

    for k in range(1, T):
        greet({"tp": (tp + k) % T})
    for k in range(1, Y):
        greet({"sp": z * Y + (y + k) % Y})
    has_up = z + 1 < Z
    has_down = z > 0
    far_up = jnp.logical_and(has_up, y == Y - 1) if Y > 1 else None
    far_down = jnp.logical_and(has_down, y == 0) if Y > 1 else None
    expect = (T - 1) + (Y - 1) + has_up.astype(jnp.int32) + has_down.astype(jnp.int32)

    @pl.when(has_up)
    def _():
        greet({"sp": sp + Y})

    @pl.when(has_down)
    def _():
        greet({"sp": sp - Y})

    if Y > 1:
        expect = expect + far_up.astype(jnp.int32) + far_down.astype(jnp.int32)

        @pl.when(far_up)
        def _():
            greet({"sp": sp + 1})

        @pl.when(far_down)
        def _():
            greet({"sp": sp - 1})

    pl.semaphore_wait(barrier, expect)

    def tok_rows(r):
        return pl.ds(pl.multiple_of(r * R, R), R)

    def tok_copy(src, piece, r, send, target):
        return pltpu.make_async_remote_copy(
            src_ref=src,
            dst_ref=tok.at[piece, tok_rows(r), :],
            send_sem=send,
            recv_sem=tok_recv.at[piece, r],
            device_id={"tp": target},
        )

    def tok_own(k, r):
        target = peer(k) if k else sib
        return tok_copy(tokens.at[tok_rows(r), :], tp, r, tok_send.at[k, r], target)

    def tok_forward(k, r):
        piece = source(k)
        return tok_copy(tok.at[piece, tok_rows(r), :], piece, r, tok_relay.at[k, r], sib)

    def tok_wait(piece, r):
        tok_copy(tok.at[piece, tok_rows(r), :], piece, r, tok_send.at[0, r], sib).wait_recv()

    for r in range(NR):
        for k in list(range(1, X)) + [0]:
            tok_own(k, r).start()

    lane = lax.broadcasted_iota(jnp.int32, (R, V), 1)
    first = (lane % hd) < (hd // 2)

    def table(r, carry):
        base = sp * L + r * R
        pos = (base + lax.broadcasted_iota(jnp.int32, (R, V), 0)).astype(F32)
        angle = pos * freq[...]
        sine = jnp.sin(angle)
        cos_t[tok_rows(r), :] = jnp.cos(angle)
        sin_t[tok_rows(r), :] = jnp.where(first, -sine, sine)
        return carry

    lax.fori_loop(0, NR, table, 0)

    def rotate(block, rows):
        low = (lax.broadcasted_iota(jnp.int32, block.shape, 1) % hd) < (hd // 2)
        other = jnp.where(
            low, pltpu.roll(block, V - hd // 2, 1), pltpu.roll(block, hd // 2, 1)
        )
        return block * cos_t[rows, :] + other * sin_t[rows, :]

    def kv_copy(j, r, send, target):
        block = kv.at[j, tok_rows(r), :]
        return pltpu.make_async_remote_copy(
            src_ref=block,
            dst_ref=block,
            send_sem=send,
            recv_sem=kv_recv.at[j, r],
            device_id={"sp": target},
        )

    def kv_up(dz, r):
        return kv_copy(sp - dz * Y, r, kv_send_z.at[dz, r], sp + Y)

    def kv_side(dz, r, k):
        return kv_copy(sp - dz * Y, r, kv_send_y.at[dz, r, k - 1], z * Y + (y + k) % Y)

    def kv_wait(j, r):
        kv_copy(j, r, kv_send_z.at[0, r], sp).wait_recv()

    EX = NR // 2 if Y == 2 else 0

    def extra(r):
        return kv_copy(0, r, kv_extra.at[r], sp + Y)

    def kv_send(dz, r, act):
        @pl.when(has_up)
        def _():
            act(kv_up(dz, r))

        for k in range(1, Y):
            wanted = jnp.logical_or(dz > 0, y + k < Y)
            if EX:
                other_way = jnp.logical_and(dz == z, jnp.logical_and(dz > 0, r < EX))
                wanted = jnp.logical_and(wanted, jnp.logical_not(jnp.logical_and(y == 0, other_way)))

            @pl.when(wanted)
            def _():
                act(kv_side(dz, r, k))

    def relay(dz, r):
        @pl.when(dz <= z)
        def _():
            kv_wait(sp - dz * Y, r)
            kv_send(dz, r, lambda copy: copy.start())

    def first_relay(r):
        relay(1, r)
        if EX:

            @pl.when(jnp.logical_and(jnp.logical_and(z == 0, y == 1), r < EX))
            def _():
                kv_wait(0, r)

                @pl.when(has_up)
                def _():
                    extra(r).start()

    own.wait()
    loads[0].wait()
    loads[1].wait()

    def key_chunk(r, carry):
        rows = tok_rows(r)
        for k in range(1, X):
            tok_wait(source(k), r)
            tok_forward(k, r).start()
        tok_wait(sib, r)
        for k in range(1, X):
            tok_wait(((xi + k) % X) * 2 + (1 - core), r)
        squares = jnp.zeros((R, 1), F32)
        for t in range(T):
            block = tok[t, rows, :].astype(F32)
            squares = squares + jnp.sum(block * block, axis=1, keepdims=True)
            scaled[rows, t * Dt : (t + 1) * Dt] = (block * gain[:, t * Dt : (t + 1) * Dt]).astype(BF16)
        inverse = lax.rsqrt(squares / Wd + NORM_EPS)
        inv[rows, :] = inverse
        left = scaled[rows, :]
        keys = inverse * dot(left, wk[...])
        for h in range(H):
            kv[sp, rows, h * V : (h + 1) * V] = rotate(keys[:, h * V : (h + 1) * V], rows).astype(BF16)
        kv[sp, rows, C : 2 * C] = (inverse * dot(left, wv[...])).astype(BF16)
        kv_send(0, r, lambda copy: copy.start())

        @pl.when(r > 0)
        def _():
            first_relay(r - 1)

        return carry

    lax.fori_loop(0, NR, key_chunk, 0)

    for load in loads[2:6]:
        load.wait()
    half = lax.broadcasted_iota(jnp.int32, (M, V), 1) < hd
    scale = hd ** (-0.5)

    def mix_rows(r):
        return pl.ds(pl.multiple_of(r * M, M), M)

    def query_chunk(r, carry):
        rows = mix_rows(r)
        inverse = inv[rows, :]
        left = scaled[rows, :]
        queries = inverse * dot(left, wq[...])
        for h in range(H):
            turned = rotate(queries[:, h * V : (h + 1) * V], rows).astype(BF16).astype(F32) * scale
            qz[h, 0, rows, :] = jnp.where(half, turned, 0.0).astype(BF16)
            qz[h, 1, rows, :] = jnp.where(half, 0.0, turned).astype(BF16)
        inner = (inverse * dot(left, wi[...])).astype(BF16)
        signal = (inverse * dot(left, ws[...])).astype(BF16)
        conv_in = (inner.astype(F32) * signal.astype(F32)).astype(BF16)
        padded[pl.ds(pl.multiple_of(PAD + r * M, PAD), M), :] = conv_in.astype(F32)
        gate[rows, :] = (inverse * dot(left, wo[...])).astype(BF16)

        @pl.when(r == 0)
        def _():
            first_relay(NR - 1)

        return carry

    lax.fori_loop(0, NM, query_chunk, 0)
    tail[...] = padded[L : L + PAD, :].astype(BF16)
    rim_copy = pltpu.make_async_remote_copy(
        src_ref=tail,
        dst_ref=rim,
        send_sem=rim_sem.at[0],
        recv_sem=rim_sem.at[1],
        device_id={"sp": (sp + 1) % S},
    )

    @pl.when(sp + 1 < S)
    def _():
        rim_copy.start()

    def attend(j, diagonal):
        def one(i, carry):
            rows = mix_rows(i)
            for h in range(H):
                query = qz[h, :, rows, :].reshape(2 * M, V)
                scores = dot_t(query, kv[j, :, h * V : (h + 1) * V])
                if diagonal:
                    row = lax.broadcasted_iota(jnp.int32, scores.shape, 0)
                    row = jnp.where(row >= M, row - M, row) + i * M
                    col = lax.broadcasted_iota(jnp.int32, scores.shape, 1)
                    scores = jnp.where(row >= col, scores, MASKED)
                    new_max = jnp.max(scores, axis=1, keepdims=True)
                else:
                    old_max = row_max[h, :, rows, :].reshape(2 * M, 1)
                    new_max = jnp.maximum(old_max, jnp.max(scores, axis=1, keepdims=True))
                weights = jnp.exp(scores - new_max)
                sums = jnp.sum(weights, axis=1, keepdims=True)
                mixed = dot(weights.astype(BF16), kv[j, :, C + h * V : C + (h + 1) * V])
                if not diagonal:
                    fade = jnp.exp(old_max - new_max)
                    sums = sums + fade * row_sum[h, :, rows, :].reshape(2 * M, 1)
                    mixed = mixed + fade * acc[h, :, rows, :].reshape(2 * M, V)
                row_max[h, :, rows, :] = new_max.reshape(2, M, 1)
                row_sum[h, :, rows, :] = sums.reshape(2, M, 1)
                acc[h, :, rows, :] = mixed.reshape(2, M, V)
            return carry

        lax.fori_loop(0, NM, one, 0)

    attend(sp, True)

    @pl.when(sp > 0)
    def _():
        rim_copy.wait_recv()
        padded[0:PAD, :] = rim[...].astype(F32)

    @pl.when(sp == 0)
    def _():
        padded[0:PAD, :] = jnp.zeros((PAD, C), F32)

    summed = jnp.zeros((L, C), F32)
    for j in range(taps_n):
        begin = PAD - (taps_n - 1) + j
        summed = summed + taps[j : j + 1, :] * padded[begin : begin + L, :]
    conv_all[tp, :, :] = (gate[...].astype(F32) * summed).astype(BF16)

    def mix_copy(which, buf, piece, r, send, target):
        block = buf.at[piece, mix_rows(r), :]
        return pltpu.make_async_remote_copy(
            src_ref=block,
            dst_ref=block,
            send_sem=send,
            recv_sem=mix_recv.at[which, piece, r],
            device_id={"tp": target},
        )

    def mix_own(which, buf, k, r):
        target = peer(k) if k else sib
        return mix_copy(which, buf, tp, r, mix_send.at[which, k, r], target)

    def mix_forward(which, buf, k, r):
        return mix_copy(which, buf, source(k), r, mix_relay.at[which, k, r], sib)

    def mix_wait(which, buf, piece, r):
        mix_copy(which, buf, piece, r, mix_send.at[which, 0, r], sib).wait_recv()

    for r in range(NM):
        for k in list(range(1, X)) + [0]:
            mix_own(0, conv_all, k, r).start()

    def step(dz, carry):
        def row_block(k, inner):
            def forward(r, c):
                relay(dz + 1, r)
                return c

            lax.fori_loop(k * NR // Y, (k + 1) * NR // Y, forward, 0)
            side = (y + k) % Y
            level = jnp.where(k == 0, z - dz, z - dz + 1)
            j = level * Y + side
            valid = jnp.where(k == 0, dz <= z, jnp.logical_or(level < z, side < y))

            @pl.when(valid)
            def _():
                @pl.when(k > 0)
                def _():
                    for r in range(NR):
                        if r < EX:
                            climbs = jnp.logical_and(level == 0, y == 1)

                            @pl.when(jnp.logical_not(jnp.logical_and(climbs, z == 0)))
                            def _():
                                kv_wait(j, r)

                            @pl.when(jnp.logical_and(climbs, jnp.logical_and(z > 0, has_up)))
                            def _():
                                extra(r).start()

                        else:
                            kv_wait(j, r)

                attend(j, False)

            return inner

        lax.fori_loop(0, Y, row_block, 0)
        return carry

    lax.fori_loop(1, z + 2, step, 0)

    def finish(i, carry):
        rows = mix_rows(i)
        for h in range(H):
            first_map = acc[h, 0, rows, :] / row_sum[h, 0, rows, :]
            second_map = acc[h, 1, rows, :] / row_sum[h, 1, rows, :]
            head_mix = first_map - lambdas[h] * second_map
            mean = jnp.mean(head_mix * head_mix, axis=1, keepdims=True)
            normed = head_mix * lax.rsqrt(mean + HEAD_EPS) * head_gain[...] * HEAD_SCALE
            attn_all[tp, rows, h * V : (h + 1) * V] = normed.astype(BF16)
        for k in list(range(1, X)) + [0]:
            mix_own(1, attn_all, k, i).start()
        return carry

    lax.fori_loop(0, NM, finish, 0)

    loads[6].wait()
    loads[7].wait()

    def gather(which, buf, r):
        for k in range(1, X):
            mix_wait(which, buf, source(k), r)
            mix_forward(which, buf, k, r).start()

    def gather_rest(which, buf, r):
        mix_wait(which, buf, sib, r)
        for k in range(1, X):
            mix_wait(which, buf, ((xi + k) % X) * 2 + (1 - core), r)

    def conv_part(r, carry):
        rows = mix_rows(r)
        gather(0, conv_all, r)
        gather_rest(0, conv_all, r)
        part = dot(conv_all[0, rows, :], wc[0:C, :])
        for t in range(1, T):
            part = part + dot(conv_all[t, rows, :], wc[t * C : (t + 1) * C, :])
        total[rows, :] = part
        return carry

    lax.fori_loop(0, NM, conv_part, 0)

    lanes = lax.broadcasted_iota(jnp.int32, (L, 128), 1)
    columns = jnp.zeros((L, 128), F32)
    for h in range(H):
        for c in range(2):
            value = row_max[h, c, :, :] + jnp.log(row_sum[h, c, :, :])
            columns = jnp.where(lanes == 2 * h + c, value, columns)
    turned_columns = jnp.transpose(columns)
    for h in range(H):
        lse[h] = turned_columns[2 * h : 2 * h + 2, :]

    def attn_part(r, carry):
        rows = mix_rows(r)
        gather(1, attn_all, r)
        gather_rest(1, attn_all, r)
        part = total[rows, :]
        for t in range(T):
            part = part + dot(attn_all[t, rows, :], wa[t * C : (t + 1) * C, :])
        out[rows, :] = part.astype(BF16)
        return carry

    lax.fori_loop(0, NM, attn_part, 0)

    for r in range(NR):
        for k in range(X):
            tok_own(k, r).wait_send()
        for k in range(1, X):
            tok_forward(k, r).wait_send()

    def drain(dz, carry):
        def inner(r, c):
            kv_send(dz, r, lambda copy: copy.wait_send())
            return c

        return lax.fori_loop(0, NR, inner, carry)

    lax.fori_loop(0, z + 1, drain, 0)
    if EX:

        @pl.when(jnp.logical_and(y == 1, has_up))
        def _():
            for r in range(EX):
                extra(r).wait_send()

    for which, buf in ((0, conv_all), (1, attn_all)):
        for r in range(NM):
            for k in range(X):
                mix_own(which, buf, k, r).wait_send()
            for k in range(1, X):
                mix_forward(which, buf, k, r).wait_send()

    @pl.when(sp + 1 < S)
    def _():
        rim_copy.wait_send()


def per_device(
    dims,
    tokens,
    norm_gain,
    query_weight,
    key_weight,
    value_weight,
    outer_gate_weight,
    inner_gate_weight,
    conv_input_weight,
    conv_taps,
    lambdas,
    head_gain,
    attn_out_weight,
    conv_out_weight,
):
    S, T, Z, Y = dims["S"], dims["T"], dims["Z"], dims["Y"]
    L, Dt = tokens.shape
    H = lambdas.shape[0]
    C = query_weight.shape[1]
    V = C // H
    hd = V // 2
    O = attn_out_weight.shape[1]
    Wd = norm_gain.shape[0]
    NR, NM, PAD = 4, 2, 16
    X = T // 2
    frequency = ROPE_BASE ** (-np.arange(hd // 2) * 2.0 / hd)
    freq = jnp.asarray(np.tile(frequency, 4)[None, :], F32)
    any_spec = pl.BlockSpec(memory_space=pl.ANY)
    vmem = pl.BlockSpec(memory_space=pltpu.VMEM)
    smem = pl.BlockSpec(memory_space=pltpu.SMEM)
    dma = pltpu.SemaphoreType.DMA
    mixed, lse = pl.pallas_call(
        functools.partial(kernel, dict(dims, H=H)),
        out_shape=(
            jax.ShapeDtypeStruct((L, O), BF16),
            jax.ShapeDtypeStruct((H, 2, L), F32),
        ),
        in_specs=[any_spec, vmem, vmem] + [any_spec] * 6 + [vmem, smem, vmem] + [any_spec] * 2,
        out_specs=(vmem, vmem),
        scratch_shapes=[
            pltpu.VMEM((T, L, Dt), BF16),
            pltpu.VMEM((L, Wd), BF16),
            pltpu.VMEM((L, 1), F32),
            pltpu.VMEM((L, V), F32),
            pltpu.VMEM((L, V), F32),
        ]
        + [pltpu.VMEM((Wd, C), BF16)] * 6
        + [pltpu.VMEM((T * C, O), BF16)] * 2
        + [
            pltpu.VMEM((S, L, 2 * C), BF16),
            pltpu.VMEM((H, 2, L, V), BF16),
            pltpu.VMEM((H, 2, L, 1), F32),
            pltpu.VMEM((H, 2, L, 1), F32),
            pltpu.VMEM((H, 2, L, V), F32),
            pltpu.VMEM((L, C), BF16),
            pltpu.VMEM((PAD + L, C), F32),
            pltpu.VMEM((PAD, C), BF16),
            pltpu.VMEM((PAD, C), BF16),
            pltpu.VMEM((T, L, C), BF16),
            pltpu.VMEM((T, L, C), BF16),
            pltpu.VMEM((L, O), F32),
            dma((8,)),
            dma,
            dma((T, NR)),
            dma((X, NR)),
            dma((X, NR)),
            dma((S, NR)),
            dma((Z, NR)),
            dma((Z, NR, max(Y - 1, 1))),
            dma((NR,)),
            dma((2,)),
            dma((2, T, NM)),
            dma((2, X, NM)),
            dma((2, X, NM)),
        ],
        compiler_params=pltpu.CompilerParams(
            collective_id=0, has_side_effects=True, vmem_limit_bytes=60 * 1024 * 1024
        ),
        name="mixer",
    )(
        tokens,
        norm_gain[None, :],
        freq,
        query_weight,
        key_weight,
        value_weight,
        outer_gate_weight,
        inner_gate_weight,
        conv_input_weight,
        conv_taps,
        lambdas,
        head_gain[None, :],
        attn_out_weight,
        conv_out_weight,
    )
    return mixed, lse


def solution(mesh):
    S, T = mesh.shape["sp"], mesh.shape["tp"]
    Y = max(d for d in range(1, S + 1) if S % d == 0 and d * d <= S)
    dims = {"S": S, "T": T, "Z": S // Y, "Y": Y}
    in_specs = (
        P("sp", "tp"),
        P(),
        P(None, "tp"),
        P(None, "tp"),
        P(None, "tp"),
        P(None, "tp"),
        P(None, "tp"),
        P(None, "tp"),
        P(None, "tp"),
        P("tp"),
        P(),
        P(None, "tp"),
        P(None, "tp"),
    )
    out_specs = (P("sp", "tp"), P("tp", None, "sp"))
    return jax.shard_map(
        functools.partial(per_device, dims),
        mesh=mesh,
        in_specs=in_specs,
        out_specs=out_specs,
        check_vma=False,
    )
```
